32 devices in a mesh: ep: 32 (over z, y, x, core).
Axes of the slice: x: 2, y: 2, z: 4, core: 2. Of those that a mesh axis runs over, the one named last changes fastest.
Arguments:
- tokens: bfloat16 [1024, 3072], P('ep'), may hold values from -6 to 6
- norm_gain: float32 [3072], replicated, may hold values from 0.1 to 1.9
- expert_ids: int32 [1024, 4], P('ep'), may hold values from 0 to 31, as said below
- expert_scores: float32 [1024, 4], P('ep'), may hold values from -100 to 180
- group_prob: float32 [1024], P('ep'), may hold values from 0.25 to 1
- gate_weight: bfloat16 [32, 3072, 384], P('ep'), may hold values from -0.109375 to 0.109375
- up_weight: bfloat16 [32, 3072, 384], P('ep'), may hold values from -0.109375 to 0.109375
- down_weight: bfloat16 [32, 384, 3072], P('ep'), may hold values from -0.3125 to 0.3125
Outputs:
- combined: bfloat16 [1024, 3072], P('ep')
The draws below stay inside these ranges and needn't reach their ends.
Inputs may be any that keep to these rules, and one draw needn't show every extreme that they name: `expert_ids`: the 4 ids of a row are different and lie in one group of 8 consecutive experts. Among the rows of one device no expert is named by more than 16 rows, and in every draw some expert is named by exactly 16 rows of one device.
All inputs are finite; a program needn't handle non-finite values.
Results may differ from the reference program's by a relative error of at most 0.0085.
Values may be sent and summed in bfloat16 or wider, within the bound.
No kernel may reach another device: no remote copies, remote signals or barrier semaphores. Data moves between devices by JAX's collectives and lax.ppermute only.
A program may use at most 128 MiB of HBM per device.

```python
import jax
import jax.numpy as jnp
from jax import lax

D = 3072
FFE = 384
GROUPS = 4
TOP_K = 4
TOK_DEV = 32
EXPERTS = 32
TOKENS = 1024
MOST = 16
N_EP = 32


def draw_expert_ids(key, part):
    blocks_count = TOKENS // TOK_DEV
    group_size = EXPERTS // GROUPS
    hot_count = (MOST - 1) * group_size // TOP_K + 1
    keys = jax.random.split(jax.random.fold_in(key, 11), 5)
    group_order = jax.random.permutation(keys[0], GROUPS)
    chosen_rank = jnp.min(jax.random.randint(keys[1], (3, blocks_count, TOK_DEV), 0, GROUPS), axis=0)
    hot_rank = jnp.min(jax.random.randint(keys[2], (3, blocks_count, 1), 0, GROUPS), axis=0)
    position = jnp.arange(TOK_DEV)[None, :]
    group_index = group_order[jnp.where(position < hot_count, hot_rank, chosen_rank)]
    earlier_mask = (group_index[:, :, None] == group_index[:, None, :]) & (jnp.arange(TOK_DEV)[None, None, :] < jnp.arange(TOK_DEV)[None, :, None])
    earlier = jnp.sum(earlier_mask.astype(jnp.int32), axis=2)
    starts = jax.random.randint(keys[3], (blocks_count, GROUPS), 0, group_size)
    start_here = jnp.take_along_axis(starts, group_index, axis=1)
    local_ids = (start_here[:, :, None] + earlier[:, :, None] * TOP_K + jnp.arange(TOP_K)[None, None, :]) % group_size
    global_ids = group_index[:, :, None] * group_size + local_ids
    return global_ids.reshape(TOKENS, TOP_K).astype(jnp.int32)


def draw_expert_scores(key, part):
    keys = jax.random.split(jax.random.fold_in(key, 23), 3)
    base_scores = jnp.clip(jax.random.normal(keys[0], (TOKENS, TOP_K), jnp.float32), -6.0, 6.0) * 1.5
    return base_scores.astype(jnp.float32)


def levels(rng, dims, shards, low, high):
    def one(axis_at, parts):
        heights = jax.random.uniform(jax.random.fold_in(jax.random.fold_in(rng, 6), axis_at), (parts,), jnp.float32, low / len(shards), high / len(shards))
        return jnp.repeat(jnp.exp(heights), dims[axis_at] // parts).reshape((-1,) + (1,) * (len(dims) - axis_at - 1))

    level = one(*shards[0])
    for cut in shards[1:]:
        level = level * one(*cut)
    return level


def gaussian(key, dims, deviation, reach, shards=(), kind=jnp.bfloat16):
    drawn = deviation * jax.random.normal(key, dims, jnp.float32)
    if shards:
        drawn = drawn * levels(key, dims, shards, -0.22, 0.18)
    return jnp.clip(drawn, -reach, reach).astype(kind)


def setup_inputs(seed: int = 0) -> dict:
    streams_of = jax.random.split(jax.random.key(seed), 9)
    return {
        "tokens": gaussian(streams_of[0], (TOKENS, D), 1.0, 6.0, ((0, 32),)),
        "norm_gain": jnp.clip(1.0 + 0.18 * jax.random.normal(streams_of[1], (D,), jnp.float32), 0.1, 1.9),
        "expert_ids": draw_expert_ids(jax.random.fold_in(streams_of[8], 71), 0),
        "expert_scores": draw_expert_scores(jax.random.fold_in(streams_of[8], 71), 0),
        "group_prob": jnp.clip(0.25 + 0.75 * jax.random.uniform(streams_of[4], (TOKENS,), jnp.float32) ** levels(streams_of[4], (TOKENS,), ((0, 32),), -0.2, 0.2), 0.25, 1.0),
        "gate_weight": gaussian(streams_of[5], (EXPERTS, D, FFE), D ** -0.5, 0.109375, ((0, 32),)),
        "up_weight": gaussian(streams_of[6], (EXPERTS, D, FFE), D ** -0.5, 0.109375, ((0, 32),)),
        "down_weight": gaussian(streams_of[7], (EXPERTS, FFE, D), FFE ** -0.5, 0.3125, ((0, 32),)),
    }


eps_norm = 1e-05

def layer_norm(tokens, norm_gain):
    values = tokens.astype(jnp.float32)
    average = lax.optimization_barrier(jnp.mean(values, axis=1, keepdims=True))
    centred = values - average
    variance = lax.optimization_barrier(jnp.mean(centred * centred, axis=1, keepdims=True))
    return (centred * lax.rsqrt(variance + eps_norm) * norm_gain[None, :]).astype(jnp.bfloat16)

def mixing_weights(expert_scores, group_prob):
    shifted = expert_scores - lax.optimization_barrier(jnp.max(expert_scores, axis=1, keepdims=True))
    exp_scores = jnp.exp(shifted)
    return exp_scores / lax.optimization_barrier(jnp.sum(exp_scores, axis=1, keepdims=True)) * group_prob[:, None]

def expert_rows(flat_rows, gate_matrix, up_matrix, down_matrix):
    gate_act = jnp.dot(flat_rows, gate_matrix, preferred_element_type=jnp.float32)
    up_act = jnp.dot(flat_rows, up_matrix, preferred_element_type=jnp.float32)
    hidden = (jax.nn.silu(gate_act) * up_act).astype(jnp.bfloat16)
    return jnp.dot(hidden, down_matrix, preferred_element_type=jnp.float32).astype(jnp.bfloat16)

def reference(tokens, norm_gain, expert_ids, expert_scores, group_prob, gate_weight, up_weight, down_weight):
    normed = layer_norm(tokens, norm_gain)
    weights_tok = mixing_weights(expert_scores, group_prob)
    capacity = N_EP * MOST
    slot_iota = jnp.arange(capacity, dtype=jnp.int32)

    def per_expert(running, expert_index):
        matches = expert_ids == expert_index
        chosen = jnp.any(matches, axis=1)
        own_weight = lax.optimization_barrier(jnp.sum(jnp.where(matches, weights_tok, 0.0), axis=1))
        slot_token = jnp.nonzero(chosen, size=capacity, fill_value=0)[0].astype(jnp.int32)
        filled = slot_iota < jnp.sum(chosen.astype(jnp.int32))
        results = expert_rows(normed[slot_token], gate_weight[expert_index], up_weight[expert_index], down_weight[expert_index])
        slot_scale = jnp.where(filled, own_weight[slot_token], 0.0)
        running = running.at[slot_token].add(slot_scale[:, None] * results.astype(jnp.float32))
        return (running, None)
    start = jnp.zeros((TOKENS, D), jnp.float32)
    mixture, _ = lax.scan(per_expert, start, jnp.arange(EXPERTS, dtype=jnp.int32))
    return mixture.astype(jnp.bfloat16)
```

```python
import functools

import jax
import jax.numpy as jnp
from jax import lax
from jax.experimental import pallas as pl
from jax.experimental.pallas import tpu as pltpu
from jax.sharding import PartitionSpec as P

GROUPS = 4
eps_norm = 1e-05

VMEM = pl.BlockSpec(memory_space=pltpu.VMEM)
f32 = jnp.float32
bf16 = jnp.bfloat16


def prepare_kernel(n, tokens_ref, gain_ref, ids_ref, scores_ref, prob_ref, out_ref, turn_ref):
    t, d = tokens_ref.shape
    k = ids_ref.shape[0]
    values = tokens_ref[...].astype(f32)
    average = jnp.mean(values, axis=1, keepdims=True)
    centred = values - average
    variance = jnp.mean(centred * centred, axis=1, keepdims=True)
    normed = centred * lax.rsqrt(variance + eps_norm) * gain_ref[...]
    out_ref[:, :d] = normed.astype(bf16)
    scores = scores_ref[...]
    exp_scores = jnp.exp(scores - jnp.max(scores, axis=0, keepdims=True))
    turn_ref[...] = jnp.zeros(turn_ref.shape, f32)
    turn_ref[:k, :t] = exp_scores / jnp.sum(exp_scores, axis=0, keepdims=True) * prob_ref[...]
    turn_ref[k : 2 * k, :t] = ids_ref[...].astype(f32)
    turned = turn_ref[...].T[:t]
    column = lax.broadcasted_iota(jnp.int32, (t, out_ref.shape[1] - d), 1)
    expert = jnp.where(column >= n, column - n, column).astype(f32)
    value = jnp.zeros(column.shape, f32)
    for j in range(k):
        value = value + jnp.where(expert == turned[:, k + j : k + j + 1], turned[:, j : j + 1], 0.0)
    high = value.astype(bf16).astype(f32)
    low = jnp.where(column < 2 * n, value - high, 0.0)
    out_ref[:, d:] = jnp.where(column < n, high, low).astype(bf16)


def prepare(tokens, norm_gain, expert_ids, expert_scores, group_prob, n):
    t, d = tokens.shape
    width = d + 2 * n + (-2 * n) % 128
    return pl.pallas_call(
        functools.partial(prepare_kernel, n),
        out_shape=jax.ShapeDtypeStruct((t, width), bf16),
        in_specs=[VMEM] * 5,
        out_specs=VMEM,
        scratch_shapes=[pltpu.VMEM((8, 128), f32)],
        compiler_params=pltpu.CompilerParams(vmem_limit_bytes=4 * 2**20),
        name="prepare",
    )(tokens, norm_gain[None, :], expert_ids.T, expert_scores.T, group_prob[None, :])


def expert_kernel(own_ref, other_ref, gate_ref, up_ref, down_ref, pick_ref, keep_ref, give_ref, x_ref, h_ref):
    m = own_ref.shape[0]
    d = keep_ref.shape[1]
    x_ref[:m] = own_ref[...]
    x_ref[m:] = other_ref[...]
    weight = jnp.sum(x_ref[:, d:].astype(f32) * pick_ref[...], axis=1, keepdims=True)
    x = x_ref[:, :d]
    gate = jnp.dot(x, gate_ref[0], preferred_element_type=f32)
    up = jnp.dot(x, up_ref[0], preferred_element_type=f32)
    h_ref[...] = (gate * jax.nn.sigmoid(gate) * up).astype(bf16)
    step = 256
    for j in range(0, d, step):
        out = jnp.dot(h_ref[...], down_ref[0, :, j : j + step], preferred_element_type=f32) * weight
        keep_ref[:, j : j + step] = out[:m]
        give_ref[:, j : j + step] = out[m:].astype(bf16)


def expert(own, other, gate_weight, up_weight, down_weight, pick):
    m, width = own.shape
    d, ffe = gate_weight.shape[1:]
    block = min(m, 128)
    weights = pl.BlockSpec(memory_space=pltpu.VMEM)
    rows = pl.BlockSpec((block, width), lambda i: (i, 0))
    outs = pl.BlockSpec((block, d), lambda i: (i, 0))
    single = m == block
    return pl.pallas_call(
        expert_kernel,
        grid=() if single else (m // block,),
        out_shape=(jax.ShapeDtypeStruct((m, d), f32), jax.ShapeDtypeStruct((m, d), bf16)),
        in_specs=[VMEM if single else rows] * 2 + [weights] * 4,
        out_specs=(VMEM, VMEM) if single else (outs, outs),
        scratch_shapes=[pltpu.VMEM((2 * block, width), bf16), pltpu.VMEM((2 * block, ffe), bf16)],
        compiler_params=pltpu.CompilerParams(vmem_limit_bytes=16 * 2**20),
        cost_estimate=pl.CostEstimate(
            flops=12 * m * d * ffe, bytes_accessed=20 * m * d, transcendentals=2 * m * ffe
        ),
        name="expert",
    )(own, other, gate_weight, up_weight, down_weight, pick)


def fold_kernel(keep_ref, got_ref, kept_ref, give_ref):
    half = kept_ref.shape[0]
    kept_ref[...] = keep_ref[:half] + got_ref[:half].astype(f32)
    give_ref[...] = (keep_ref[half:] + got_ref[half:].astype(f32)).astype(bf16)


def fold(keep, got):
    m, d = keep.shape
    block = min(m // 2, 128)
    if block * 2 == m:
        return pl.pallas_call(
            fold_kernel,
            out_shape=(
                jax.ShapeDtypeStruct((m // 2, d), f32),
                jax.ShapeDtypeStruct((m // 2, d), bf16),
            ),
            in_specs=[VMEM, VMEM],
            out_specs=(VMEM, VMEM),
            compiler_params=pltpu.CompilerParams(vmem_limit_bytes=4 * 2**20),
            cost_estimate=pl.CostEstimate(flops=m * d * 64, bytes_accessed=12 * m * d, transcendentals=0),
            name="fold",
        )(keep, got)
    total = keep + got.astype(f32)
    return total[: m // 2], total[m // 2 :].astype(bf16)


def local(
    tokens, norm_gain, expert_ids, expert_scores, group_prob, gate_weight, up_weight, down_weight
):
    n = lax.axis_size("ep")
    size = n // GROUPS
    _, d = tokens.shape
    bits = [1 << b for b in range(1, size.bit_length() - 1)]
    me = lax.axis_index("ep")

    def exchange(x, flip):
        return lax.ppermute(x, "ep", [(i, i ^ flip(i)) for i in range(n)])

    def plane(step):
        return lambda i: bits[step] if i % 2 == 0 else bits[-1 - step]

    def group(q):
        return lambda i: q * size

    sent = prepare(tokens, norm_gain, expert_ids, expert_scores, group_prob, n)
    columns = jnp.arange(sent.shape[1] - d)[None, :]
    pick = ((columns == me) | (columns == n + me)).astype(f32)
    shard = [sent, exchange(sent, group(1)), exchange(sent, group(2)), None]
    shard[3] = exchange(shard[2], group(1))
    parts = []
    for q in range(GROUPS):
        x = shard[q]
        for s in range(len(bits)):
            x = jnp.concatenate([x, exchange(x, plane(s))], axis=0)
        other = exchange(x, lambda i: 1)
        keep, give = expert(x, other, gate_weight, up_weight, down_weight, pick)
        got = exchange(give, lambda i: 1)
        for s in reversed(range(len(bits))):
            keep, give = fold(keep, got)
            got = exchange(give, plane(s))
        part = keep + got.astype(f32)
        if q:
            part = exchange(part.astype(bf16), group(q)).astype(f32)
        parts.append(part)
    return (parts[0] + parts[1] + parts[2] + parts[3]).astype(bf16)


def solution(mesh):
    in_specs = (
        P("ep", None), P(), P("ep", None), P("ep", None), P("ep"),
        P("ep", None, None), P("ep", None, None), P("ep", None, None),
    )

    return jax.shard_map(local, mesh=mesh, in_specs=in_specs, out_specs=P("ep", None), check_vma=False)
```

```python
import functools

import jax
import jax.numpy as jnp
from jax import lax
from jax.experimental import pallas as pl
from jax.experimental.pallas import tpu as pltpu
from jax.sharding import PartitionSpec as P


GROUPS = 4
eps_norm = 1e-05


VMEM = pl.BlockSpec(memory_space=pltpu.VMEM)
f32 = jnp.float32
bf16 = jnp.bfloat16


def prepare_kernel(n, *refs):
    sources, out_ref, turn_ref, copies, sems = refs[:5], refs[5], refs[6], refs[7:12], refs[12]
    moves = [pltpu.make_async_copy(a, b, sems.at[i]) for i, (a, b) in enumerate(zip(sources, copies))]
    for move in moves:
        move.start()
    for move in moves:
        move.wait()
    tokens_ref, gain_ref, ids_ref, scores_ref, prob_ref = copies
    t, d = tokens_ref.shape
    k = ids_ref.shape[0]
    values = tokens_ref[...].astype(f32)
    average = jnp.mean(values, axis=1, keepdims=True)
    centred = values - average
    variance = jnp.mean(centred * centred, axis=1, keepdims=True)
    normed = centred * lax.rsqrt(variance + eps_norm) * gain_ref[...]
    out_ref[:, :d] = normed.astype(bf16)
    scores = scores_ref[...]
    exp_scores = jnp.exp(scores - jnp.max(scores, axis=0, keepdims=True))
    turn_ref[...] = jnp.zeros(turn_ref.shape, f32)
    turn_ref[:k, :t] = exp_scores / jnp.sum(exp_scores, axis=0, keepdims=True) * prob_ref[...]
    turn_ref[k : 2 * k, :t] = ids_ref[...].astype(f32)
    turned = turn_ref[...].T[:t]
    column = lax.broadcasted_iota(jnp.int32, (t, out_ref.shape[1] - d), 1)
    expert = jnp.where(column >= n, column - n, column).astype(f32)
    value = jnp.zeros(column.shape, f32)
    for j in range(k):
        value = value + jnp.where(expert == turned[:, k + j : k + j + 1], turned[:, j : j + 1], 0.0)
    high = value.astype(bf16).astype(f32)
    low = jnp.where(column < 2 * n, value - high, 0.0)
    out_ref[:, d:] = jnp.where(column < n, high, low).astype(bf16)


def prepare(tokens, norm_gain, expert_ids, expert_scores, group_prob, n):
    t, d = tokens.shape
    width = d + 2 * n + (-2 * n) % 128
    arrays = (tokens, norm_gain[None, :], expert_ids.T, expert_scores.T, group_prob[None, :])
    return pl.pallas_call(
        functools.partial(prepare_kernel, n),
        out_shape=jax.ShapeDtypeStruct((t, width), bf16),
        in_specs=[pl.BlockSpec(memory_space=pltpu.HBM)] * 5,
        out_specs=VMEM,
        scratch_shapes=[pltpu.VMEM((8, 128), f32)]
        + [pltpu.VMEM(a.shape, a.dtype) for a in arrays]
        + [pltpu.SemaphoreType.DMA((5,))],
        compiler_params=pltpu.CompilerParams(vmem_limit_bytes=4 * 2**20),
        name="prepare",
    )(*(pltpu.with_memory_space_constraint(a, pltpu.HBM) for a in arrays))


def expert_kernel(n, own_ref, other_ref, gate_ref, up_ref, down_ref, keep_ref, give_ref, x_ref, h_ref):
    m = own_ref.shape[0]
    d = keep_ref.shape[1]
    x_ref[:m] = own_ref[...]
    x_ref[m:] = other_ref[...]
    me = lax.axis_index("ep")
    columns = x_ref[:, d:].astype(f32)
    index = lax.broadcasted_iota(jnp.int32, columns.shape, 1)
    mine = (index == me) | (index == n + me)
    weight = jnp.sum(jnp.where(mine, columns, 0.0), axis=1, keepdims=True)
    x = x_ref[:, :d]
    gate = jnp.dot(x, gate_ref[0], preferred_element_type=f32)
    up = jnp.dot(x, up_ref[0], preferred_element_type=f32)
    h_ref[...] = (gate * jax.nn.sigmoid(gate) * up).astype(bf16)
    step = 256
    for j in range(0, d, step):
        out = jnp.dot(h_ref[...], down_ref[0, :, j : j + step], preferred_element_type=f32) * weight
        keep_ref[:, j : j + step] = out[:m]
        give_ref[:, j : j + step] = out[m:].astype(bf16)


def expert(own, other, gate_weight, up_weight, down_weight, n):
    m, width = own.shape
    d, ffe = gate_weight.shape[1:]
    block = min(m, 128)
    weights = pl.BlockSpec(memory_space=pltpu.VMEM)
    rows = pl.BlockSpec((block, width), lambda i: (i, 0))
    outs = pl.BlockSpec((block, d), lambda i: (i, 0))
    single = m == block
    return pl.pallas_call(
        functools.partial(expert_kernel, n),
        grid=() if single else (m // block,),
        out_shape=(jax.ShapeDtypeStruct((m, d), f32), jax.ShapeDtypeStruct((m, d), bf16)),
        in_specs=[VMEM if single else rows] * 2 + [weights] * 3,
        out_specs=(VMEM, VMEM) if single else (outs, outs),
        scratch_shapes=[pltpu.VMEM((2 * block, width), bf16), pltpu.VMEM((2 * block, ffe), bf16)],
        compiler_params=pltpu.CompilerParams(vmem_limit_bytes=16 * 2**20),
        cost_estimate=pl.CostEstimate(
            flops=12 * m * d * ffe, bytes_accessed=20 * m * d, transcendentals=2 * m * ffe
        ),
        name="expert",
    )(own, other, gate_weight, up_weight, down_weight)


def join_kernel(low_ref, high_ref, out_ref):
    half = low_ref.shape[0]
    out_ref[:half] = low_ref[...]
    out_ref[half:] = high_ref[...]


def join(low, high):
    m, width = low.shape
    if m > 128:
        return jnp.concatenate([low, high], axis=0)
    return pl.pallas_call(
        join_kernel,
        out_shape=jax.ShapeDtypeStruct((2 * m, width), low.dtype),
        in_specs=[VMEM] * 2,
        out_specs=VMEM,
        compiler_params=pltpu.CompilerParams(vmem_limit_bytes=4 * 2**20),
        cost_estimate=pl.CostEstimate(flops=m * width * 64, bytes_accessed=8 * m * width, transcendentals=0),
        name="join",
    )(low, high)


def merge_kernel(*refs):
    *added, out_ref = refs
    total = added[0][...].astype(f32)
    for ref in added[1:]:
        total = total + ref[...].astype(f32)
    out_ref[...] = total.astype(bf16)


def merge(*arrays):
    m, d = arrays[0].shape
    if m > 256:
        return sum(a.astype(f32) for a in arrays).astype(bf16)
    return pl.pallas_call(
        merge_kernel,
        out_shape=jax.ShapeDtypeStruct((m, d), bf16),
        in_specs=[VMEM] * len(arrays),
        out_specs=VMEM,
        compiler_params=pltpu.CompilerParams(vmem_limit_bytes=4 * 2**20),
        cost_estimate=pl.CostEstimate(flops=m * d * 64, bytes_accessed=10 * m * d, transcendentals=0),
        name="merge",
    )(*arrays)


def fold_kernel(*refs):
    *added, kept_ref, give_ref = refs
    half = kept_ref.shape[0]
    low = added[0][:half].astype(f32)
    high = added[0][half:].astype(f32)
    for ref in added[1:]:
        low = low + ref[:half].astype(f32)
        high = high + ref[half:].astype(f32)
    kept_ref[...] = low
    give_ref[...] = high.astype(bf16)


def fold(*arrays):
    m, d = arrays[0].shape
    half = m // 2
    if m <= 256:
        return pl.pallas_call(
            fold_kernel,
            out_shape=(jax.ShapeDtypeStruct((half, d), f32), jax.ShapeDtypeStruct((half, d), bf16)),
            in_specs=[VMEM] * len(arrays),
            out_specs=(VMEM, VMEM),
            compiler_params=pltpu.CompilerParams(vmem_limit_bytes=4 * 2**20),
            cost_estimate=pl.CostEstimate(flops=m * d * 64, bytes_accessed=12 * m * d, transcendentals=0),
            name="fold",
        )(*arrays)
    total = sum(a.astype(f32) for a in arrays)
    return total[:half], total[half:].astype(bf16)


def local(
    tokens, norm_gain, expert_ids, expert_scores, group_prob, gate_weight, up_weight, down_weight
):
    n = lax.axis_size("ep")
    size = n // GROUPS
    bits = [1 << b for b in range(1, size.bit_length() - 1)]

    def exchange(x, flip):
        return lax.ppermute(x, "ep", [(i, i ^ flip(i)) for i in range(n)])

    def plane(step):
        return lambda i: bits[step] if i % 2 == 0 else bits[-1 - step]

    def group(q):
        return lambda i: q * size

    sent = prepare(tokens, norm_gain, expert_ids, expert_scores, group_prob, n)
    first, rows = {0: sent}, {}
    first[1] = exchange(sent, group(1))
    first[2] = exchange(sent, group(2))
    first[3] = exchange(first[2], group(1))
    for q in range(GROUPS):
        x = first[q]
        for s in range(len(bits)):
            y = exchange(x, plane(s))
            x = join(x, y)
        rows[q] = x
    keep, got = {}, {}
    for q in range(GROUPS):
        other = exchange(rows[q], lambda i: 1)
        keep[q], give = expert(rows[q], other, gate_weight, up_weight, down_weight, n)
        got[q] = exchange(give, lambda i: 1)
    parts = []
    for q in (1, 2, 3, 0):
        kept, extra = keep[q], got[q]
        for s in reversed(range(len(bits))):
            kept, give = fold(kept, extra)
            extra = exchange(give, plane(s))
        if q:
            part = merge(kept, extra)
            parts.append(exchange(part, group(q)))
    return merge(kept, extra, *parts)


def solution(mesh):
    in_specs = (
        P("ep", None), P(), P("ep", None), P("ep", None), P("ep"),
        P("ep", None, None), P("ep", None, None), P("ep", None, None),
    )

    return jax.shard_map(local, mesh=mesh, in_specs=in_specs, out_specs=P("ep", None), check_vma=False)
```

```python
import functools

import jax
import jax.numpy as jnp
from jax import lax
from jax.experimental import pallas as pl
from jax.experimental.pallas import tpu as pltpu
from jax.sharding import PartitionSpec as P

GROUPS = 4
eps_norm = 1e-05
CUT_OUT = 1
CUT_BACK = 1
NEAR_STEPS = 2

VMEM = pl.BlockSpec(memory_space=pltpu.VMEM)
f32 = jnp.float32
bf16 = jnp.bfloat16


def small(kernel, outs, arrays, limit=4, scratch=()):
    work = sum(a.size for a in arrays)
    return pl.pallas_call(
        kernel,
        out_shape=outs,
        in_specs=[VMEM] * len(arrays),
        out_specs=jax.tree.map(lambda _: VMEM, outs),
        scratch_shapes=scratch,
        compiler_params=pltpu.CompilerParams(vmem_limit_bytes=limit * 2**20),
        cost_estimate=pl.CostEstimate(flops=work, bytes_accessed=4 * work, transcendentals=0),
    )(*arrays)


def prepare_body(n, parts, *refs):
    sources, outs, turn_ref = refs[:5], refs[5 : 5 + parts], refs[5 + parts]
    copies, sems = refs[6 + parts : 11 + parts], refs[11 + parts]
    moves = [pltpu.make_async_copy(a, b, sems.at[i]) for i, (a, b) in enumerate(zip(sources, copies))]
    for move in moves:
        move.start()
    for move in moves:
        move.wait()
    tokens_ref, gain_ref, ids_ref, scores_ref, prob_ref = copies
    out_ref = outs[0]
    t, d = tokens_ref.shape
    k = ids_ref.shape[0]
    values = tokens_ref[...].astype(f32)
    average = jnp.mean(values, axis=1, keepdims=True)
    centred = values - average
    variance = jnp.mean(centred * centred, axis=1, keepdims=True)
    normed = centred * lax.rsqrt(variance + eps_norm) * gain_ref[...]
    out_ref[:, :d] = normed.astype(bf16)
    scores = scores_ref[...]
    exp_scores = jnp.exp(scores - jnp.max(scores, axis=0, keepdims=True))
    turn_ref[...] = jnp.zeros(turn_ref.shape, f32)
    turn_ref[:k, :t] = exp_scores / jnp.sum(exp_scores, axis=0, keepdims=True) * prob_ref[...]
    turn_ref[k : 2 * k, :t] = ids_ref[...].astype(f32)
    turned = turn_ref[...].T[:t]
    column = lax.broadcasted_iota(jnp.int32, (t, out_ref.shape[1] - d), 1)
    expert = jnp.where(column >= n, column - n, column).astype(f32)
    value = jnp.zeros(column.shape, f32)
    for j in range(k):
        value = value + jnp.where(expert == turned[:, k + j : k + j + 1], turned[:, j : j + 1], 0.0)
    high = value.astype(bf16).astype(f32)
    low = jnp.where(column < 2 * n, value - high, 0.0)
    out_ref[:, d:] = jnp.where(column < n, high, low).astype(bf16)
    if parts > 1:
        piece = t // (parts - 1)
        for i, ref in enumerate(outs[1:]):
            ref[...] = out_ref[i * piece : (i + 1) * piece]


def prepare(tokens, norm_gain, expert_ids, expert_scores, group_prob, n):
    t, d = tokens.shape
    width = d + 2 * n + (-2 * n) % 128
    outs = [jax.ShapeDtypeStruct((t, width), bf16)]
    if CUT_OUT > 1:
        outs += [jax.ShapeDtypeStruct((t // CUT_OUT, width), bf16)] * CUT_OUT
    arrays = (tokens, norm_gain[None, :], expert_ids.T, expert_scores.T, group_prob[None, :])
    out = pl.pallas_call(
        functools.partial(prepare_body, n, len(outs)),
        out_shape=tuple(outs),
        in_specs=[pl.BlockSpec(memory_space=pltpu.HBM)] * 5,
        out_specs=(VMEM,) * len(outs),
        scratch_shapes=[pltpu.VMEM((8, 128), f32)]
        + [pltpu.VMEM(a.shape, a.dtype) for a in arrays]
        + [pltpu.SemaphoreType.DMA((5,))],
        compiler_params=pltpu.CompilerParams(vmem_limit_bytes=4 * 2**20),
        name="prepare",
    )(*(pltpu.with_memory_space_constraint(a, pltpu.HBM) for a in arrays))
    return out[0], out[1:] if CUT_OUT > 1 else out


def expert_kernel(n, takes, gives, *refs):
    pieces, (gate_ref, up_ref, down_ref) = refs[: 2 * takes], refs[2 * takes : 2 * takes + 3]
    keeps, sends = refs[2 * takes + 3 :][:gives], refs[2 * takes + 3 + gives :][:gives]
    x_ref, h_ref = refs[-2:]
    d = keeps[0].shape[1]
    at = 0
    for ref in pieces:
        x_ref[at : at + ref.shape[0]] = ref[...]
        at += ref.shape[0]
    m = at // 2
    me = lax.axis_index("ep")
    columns = x_ref[:, d:].astype(f32)
    index = lax.broadcasted_iota(jnp.int32, columns.shape, 1)
    mine = (index == me) | (index == n + me)
    weight = jnp.sum(jnp.where(mine, columns, 0.0), axis=1, keepdims=True)
    x = x_ref[:, :d]
    gate = jnp.dot(x, gate_ref[0], preferred_element_type=f32)
    up = jnp.dot(x, up_ref[0], preferred_element_type=f32)
    h_ref[...] = (gate * jax.nn.sigmoid(gate) * up).astype(bf16)
    step = 256
    piece = m // gives
    for j in range(0, d, step):
        out = jnp.dot(h_ref[...], down_ref[0, :, j : j + step], preferred_element_type=f32) * weight
        for i in range(gives):
            keeps[i][:, j : j + step] = out[i * piece : (i + 1) * piece]
            sends[i][:, j : j + step] = out[m + i * piece : m + (i + 1) * piece].astype(bf16)


def expert(own, other, weights, n, gives):
    m = sum(a.shape[0] for a in own)
    width = own[0].shape[1]
    d, ffe = weights[0].shape[1:]
    if m > 128:
        own, other = ([jnp.concatenate(a)] for a in (own, other))
    block = min(m, 128)
    cost = pl.CostEstimate(
        flops=12 * m * d * ffe, bytes_accessed=20 * m * d, transcendentals=2 * m * ffe
    )
    scratch = [pltpu.VMEM((2 * block, width), bf16), pltpu.VMEM((2 * block, ffe), bf16)]
    params = pltpu.CompilerParams(vmem_limit_bytes=16 * 2**20)
    if m == block:
        outs = [jax.ShapeDtypeStruct((m // gives, d), f32)] * gives
        outs += [jax.ShapeDtypeStruct((m // gives, d), bf16)] * gives
        out = pl.pallas_call(
            functools.partial(expert_kernel, n, len(own), gives),
            out_shape=tuple(outs),
            in_specs=[VMEM] * (2 * len(own) + 3),
            out_specs=(VMEM,) * (2 * gives),
            scratch_shapes=scratch,
            compiler_params=params,
            cost_estimate=cost,
            name="expert",
        )(*own, *other, *weights)
        return out[:gives], out[gives:]
    rows = pl.BlockSpec((block, width), lambda i: (i, 0))
    outs = pl.BlockSpec((block, d), lambda i: (i, 0))
    keep, give = pl.pallas_call(
        functools.partial(expert_kernel, n, 1, 1),
        grid=(m // block,),
        out_shape=(jax.ShapeDtypeStruct((m, d), f32), jax.ShapeDtypeStruct((m, d), bf16)),
        in_specs=[rows] * 2 + [VMEM] * 3,
        out_specs=(outs, outs),
        scratch_shapes=scratch,
        compiler_params=params,
        cost_estimate=cost,
        name="expert",
    )(*own, *other, *weights)
    return jnp.split(keep, gives), jnp.split(give, gives)


def load_kernel(*refs):
    sems = refs[-1]
    half = (len(refs) - 1) // 2
    moves = [
        pltpu.make_async_copy(a, b, sems.at[i])
        for i, (a, b) in enumerate(zip(refs[:half], refs[half:-1]))
    ]
    for move in moves:
        move.start()
    for move in moves:
        move.wait()


def load(*arrays):
    return pl.pallas_call(
        load_kernel,
        out_shape=tuple(jax.ShapeDtypeStruct(a.shape, a.dtype) for a in arrays),
        in_specs=[pl.BlockSpec(memory_space=pltpu.HBM)] * len(arrays),
        out_specs=(VMEM,) * len(arrays),
        scratch_shapes=[pltpu.SemaphoreType.DMA((len(arrays),))],
        compiler_params=pltpu.CompilerParams(vmem_limit_bytes=16 * 2**20),
        cost_estimate=pl.CostEstimate(flops=10**6, bytes_accessed=10**7, transcendentals=0),
        name="load",
    )(*(pltpu.with_memory_space_constraint(a, pltpu.HBM) for a in arrays))


def join_kernel(*refs):
    *parts, out_ref = refs
    at = 0
    for ref in parts:
        out_ref[at : at + ref.shape[0]] = ref[...]
        at += ref.shape[0]


def join(*arrays):
    m = sum(a.shape[0] for a in arrays)
    if len(arrays) == 1:
        return arrays[0]
    if m > 256:
        return jnp.concatenate(arrays)
    out = jax.ShapeDtypeStruct((m, arrays[0].shape[1]), bf16)
    return small(join_kernel, out, arrays)


def fold_kernel(*refs):
    *added, kept_ref, give_ref = refs
    half = kept_ref.shape[0]
    low = added[0][:half].astype(f32)
    high = added[0][half:].astype(f32)
    for ref in added[1:]:
        low = low + ref[:half].astype(f32)
        high = high + ref[half:].astype(f32)
    kept_ref[...] = low
    give_ref[...] = high.astype(bf16)


def fold(*arrays):
    m, d = arrays[0].shape
    half = m // 2
    if m <= 256:
        outs = (jax.ShapeDtypeStruct((half, d), f32), jax.ShapeDtypeStruct((half, d), bf16))
        return small(fold_kernel, outs, arrays)
    total = sum(a.astype(f32) for a in arrays)
    return total[:half], total[half:].astype(bf16)


def merge_kernel(full, *refs):
    *added, out_ref = refs
    parts = len(added) - full
    piece = out_ref.shape[0] // max(parts, 1)
    for i in range(max(parts, 1)):
        rows = slice(i * piece, (i + 1) * piece)
        total = added[0][rows].astype(f32)
        for ref in added[1:full]:
            total = total + ref[rows].astype(f32)
        if parts:
            total = total + added[full + i][...].astype(f32)
        out_ref[rows] = total.astype(bf16)


def merge(*arrays, cut=()):
    m, d = arrays[0].shape
    if m > 256:
        return sum(a.astype(f32) for a in arrays).astype(bf16)
    kernel = functools.partial(merge_kernel, len(arrays))
    return small(kernel, jax.ShapeDtypeStruct((m, d), bf16), arrays + tuple(cut))


def local(
    tokens, norm_gain, expert_ids, expert_scores, group_prob, gate_weight, up_weight, down_weight
):
    n = lax.axis_size("ep")
    size = n // GROUPS
    bits = [1 << b for b in range(1, size.bit_length() - 1)]
    steps = len(bits)
    near_steps = min(NEAR_STEPS, steps)
    weights = load(gate_weight, up_weight, down_weight)

    def exchange(x, flip):
        return lax.ppermute(x, "ep", [(i, i ^ flip(i)) for i in range(n)])

    def plane(step):
        return lambda i: bits[step] if i % 2 == 0 else bits[-1 - step]

    def group(q):
        return lambda i: q * size

    def spread(x):
        for s in range(steps):
            y = exchange(x, plane(s))
            x = join(x, y)
        return x, exchange(x, lambda i: 1)

    def gather(kept, extra, stop=0, near=None):
        extra = (extra,)
        for s in reversed(range(stop, steps)):
            if near is not None and s == steps - 1 - near_steps:
                extra += (near,)
            kept, give = fold(kept, *extra)
            extra = (exchange(give, plane(s)),)
        return kept, extra

    sent, cut = prepare(tokens, norm_gain, expert_ids, expert_scores, group_prob, n)
    far2 = [exchange(x, group(2)) for x in cut]
    far3 = [exchange(x, group(1)) for x in far2]
    far2 = join(*far2)
    first = [[sent], [exchange(sent, group(1))], [far2], far3]
    keep, got = [], []
    for q in range(GROUPS):
        pairs = [spread(x) for x in first[q]]
        gives = CUT_BACK if q == 3 else 1
        kept, give = expert([a for a, _ in pairs], [b for _, b in pairs], weights, n, gives)
        keep.append(kept)
        got.append([exchange(x, lambda i: 1) for x in give])
    parts = []
    kept, extra = gather(keep[1][0], got[1][0], steps - near_steps)
    part = merge(kept, *extra)
    near = exchange(part, group(1))
    kept, extra = gather(keep[2][0], got[2][0])
    part = merge(kept, *extra)
    parts.append(exchange(part, group(2)))
    last = []
    for i in range(CUT_BACK):
        kept, extra = gather(keep[3][i], got[3][i])
        part = merge(kept, *extra)
        last.append(exchange(part, group(3)))
    whole = near_steps == steps
    kept, extra = gather(keep[0][0], got[0][0], 0, None if whole else near)
    if whole:
        parts.append(near)
    if CUT_BACK == 1:
        return merge(kept, *extra, *parts, *last)
    return merge(kept, *extra, *parts, cut=last)


def solution(mesh):
    in_specs = (
        P("ep", None), P(), P("ep", None), P("ep", None), P("ep"),
        P("ep", None, None), P("ep", None, None), P("ep", None, None),
    )

    return jax.shard_map(local, mesh=mesh, in_specs=in_specs, out_specs=P("ep", None), check_vma=False)
```
